512 devices in a mesh: fs: 64 (over z, y), tp: 8 (over x, core).
Axes of the slice: x: 4, y: 8, z: 8, core: 2. Of those that a mesh axis runs over, the one named last changes fastest.
Arguments:
- normed: bfloat16 [65536, 2048], P('fs'), may hold values from -6 to 6
- key_cot: bfloat16 [65536, 1024], P('fs', 'tp'), may hold values from -130 to 130
- value_cot: bfloat16 [65536, 2048], P('fs', 'tp'), may hold values from -130 to 130
- basis: bfloat16 [2048, 256], P('fs'), may hold values from -3.535534 to 3.535534
- master_key: float32 [2048, 1024], P('fs', 'tp'), may hold values from -3 to 3
- master_value: float32 [2048, 2048], P('fs', 'tp'), may hold values from -3 to 3
- first_key: float32 [256, 1024], P('fs', 'tp'), may hold values from -3 to 3
- second_key: float32 [256, 1024], P('fs', 'tp'), may hold values from 0.05 to 2
- first_value: float32 [256, 2048], P('fs', 'tp'), may hold values from -3 to 3
- second_value: float32 [256, 2048], P('fs', 'tp'), may hold values from 0.05 to 2
Outputs:
- step_key: float32 [2048, 1024], P('fs', 'tp')
- step_value: float32 [2048, 2048], P('fs', 'tp')
- new_master_key: float32 [2048, 1024], P('fs', 'tp')
- new_master_value: float32 [2048, 2048], P('fs', 'tp')
- copy_key: bfloat16 [2048, 1024], P(None, 'tp')
- copy_value: bfloat16 [2048, 2048], P(None, 'tp')
- new_first_key: float32 [256, 1024], P('fs', 'tp')
- new_second_key: float32 [256, 1024], P('fs', 'tp')
- new_first_value: float32 [256, 2048], P('fs', 'tp')
- new_second_value: float32 [256, 2048], P('fs', 'tp')
The draws below stay inside these ranges and needn't reach their ends.
All inputs are finite; a program needn't handle non-finite values.
Results may differ from the reference program's by a relative error of at most 0.0055.
Values may be sent and summed in bfloat16 or wider, within the bound.
A program may use at most 64 MiB of HBM per device.

```python
import math
import jax
import jax.numpy as jnp
from jax import lax

D = 2048
DK = 1024
DV = 2048
R = 256
TOKENS = 65536


def column_scaled(key, height, width):
    keys = jax.random.split(key, 2)
    ramp = jnp.arange(width, dtype=jnp.float32) / max(width - 1, 1)
    jitter = jnp.exp(jax.random.uniform(keys[1], (width,), jnp.float32, math.log(0.7), math.log(1.4)))
    scales = 10.0 ** ramp * jitter
    base_values = jnp.clip(jax.random.normal(keys[0], (height, width), jnp.float32), -6.0, 6.0)
    return base_values * scales[None, :]


def draw_basis(key, part):
    values = column_scaled(jax.random.fold_in(key, 11), D, R) * D ** (-0.5)
    return values.astype(jnp.bfloat16)


def draw_key_cot(key, part):
    return column_scaled(jax.random.fold_in(key, 12), TOKENS, DK).astype(jnp.bfloat16)


def draw_value_cot(key, part):
    return column_scaled(jax.random.fold_in(key, 13), TOKENS, DV).astype(jnp.bfloat16)


def shard_levels(stream_key, dims, cuts, low, largest):
    factor_of, own = 1.0, jax.random.fold_in(stream_key, 6)
    for dim, blocks in cuts:
        steps = jnp.exp(jax.random.uniform(jax.random.fold_in(own, dim), (blocks,), jnp.float32, low / len(cuts), largest / len(cuts)))
        factor_of = factor_of * jnp.repeat(steps, dims[dim] // blocks).reshape([-1 if axis == dim else 1 for axis in range(len(dims))])
    return factor_of


def noise(stream_key, extent, deviation, limit, cuts=(), kind=jnp.bfloat16):
    gain = shard_levels(stream_key, extent, cuts, -0.22, 0.18) if cuts else 1.0
    drawn = jax.random.normal(stream_key, extent, jnp.float32) * deviation * gain
    return jnp.minimum(jnp.maximum(drawn, -limit), limit).astype(kind)


def setup_inputs(seed: int = 0) -> dict:
    arg_keys = jax.random.split(jax.random.key(seed), 11)
    return {
        "normed": noise(arg_keys[0], (TOKENS, D), 1.0, 6.0, ((0, 64),)),
        "key_cot": draw_key_cot(jax.random.fold_in(arg_keys[10], 71), 0),
        "value_cot": draw_value_cot(jax.random.fold_in(arg_keys[10], 71), 0),
        "basis": draw_basis(jax.random.fold_in(arg_keys[10], 71), 0),
        "master_key": noise(arg_keys[4], (D, DK), 0.5, 3.0, ((0, 64), (1, 8)), jnp.float32),
        "master_value": noise(arg_keys[5], (D, DV), 0.5, 3.0, ((0, 64), (1, 8)), jnp.float32),
        "first_key": noise(arg_keys[6], (R, DK), 0.5, 3.0, ((0, 64), (1, 8)), jnp.float32),
        "second_key": jnp.clip(jnp.exp(math.log(2.0) - 3.6888794 * jax.random.uniform(arg_keys[7], (R, DK), jnp.float32) ** shard_levels(arg_keys[7], (R, DK), ((0, 64), (1, 8)), -0.2, 0.2)), 0.05, 2.0),
        "first_value": noise(arg_keys[8], (R, DV), 0.5, 3.0, ((0, 64), (1, 8)), jnp.float32),
        "second_value": jnp.clip(jnp.exp(math.log(2.0) - 3.6888794 * jax.random.uniform(arg_keys[9], (R, DV), jnp.float32) ** shard_levels(arg_keys[9], (R, DV), ((0, 64), (1, 8)), -0.2, 0.2)), 0.05, 2.0),
    }


learn_rate = 0.05
beta_first = 0.9
beta_second = 0.9
epsilon = 1e-08
norm_eps = 1e-06

def moment_update(low_grad, grad_scale, first_moment, second_moment, basis):
    scaled = low_grad * grad_scale
    new_first = beta_first * first_moment + (1.0 - beta_first) * scaled
    new_second = beta_second * second_moment + (1.0 - beta_second) * scaled * scaled
    direction = (new_first / (jnp.sqrt(new_second) + epsilon)).astype(jnp.bfloat16)
    update_step = jnp.dot(basis, direction, preferred_element_type=jnp.float32)
    return (update_step, new_first, new_second)

def reference(normed, key_cot, value_cot, basis, master_key, master_value, first_key, second_key, first_value, second_value):
    grad_key = jnp.dot(normed.T, key_cot, preferred_element_type=jnp.float32)
    grad_value = jnp.dot(normed.T, value_cot, preferred_element_type=jnp.float32)
    basis_wide = basis.astype(jnp.float32).T
    low_key = jnp.dot(basis_wide, grad_key, precision=lax.Precision.HIGHEST, preferred_element_type=jnp.float32)
    low_value = jnp.dot(basis_wide, grad_value, precision=lax.Precision.HIGHEST, preferred_element_type=jnp.float32)
    squares = jnp.sum(low_key * low_key) + jnp.sum(low_value * low_value)
    root_mean = jnp.sqrt(squares / (R * (DK + DV)) + norm_eps)
    grad_scale = 1.0 / root_mean
    step_key, new_first_key, new_second_key = moment_update(low_key, grad_scale, first_key, second_key, basis)
    step_value, new_first_value, new_second_value = moment_update(low_value, grad_scale, first_value, second_value, basis)
    new_master_key = master_key - learn_rate * step_key
    new_master_value = master_value - learn_rate * step_value
    return (step_key, step_value, new_master_key, new_master_value, new_master_key.astype(jnp.bfloat16), new_master_value.astype(jnp.bfloat16), new_first_key, new_second_key, new_first_value, new_second_value)
```

```python
import functools

import jax
import jax.numpy as jnp
from jax import lax
from jax.experimental import pallas as pl
from jax.experimental.pallas import tpu as pltpu
from jax.sharding import Mesh
from jax.sharding import PartitionSpec as P

AXES = ("z", "y", "x", "c")
FS = ("z", "y")
TP = ("x", "c")
MESH = pl.DeviceIdType.MESH
VMEM = pltpu.VMEM
DMA = pltpu.SemaphoreType.DMA
BF = jnp.bfloat16
F32 = jnp.float32

learn_rate = 0.05
beta_first = 0.9
beta_second = 0.9
epsilon = 1e-08
norm_eps = 1e-06


def permutation(n, c, rank):
    rows = lax.broadcasted_iota(jnp.int32, (rank, rank), 0)
    cols = lax.broadcasted_iota(jnp.int32, (rank, rank), 1)
    r = rows % 4
    low = (rows // 4) % n
    high = rows // (4 * n)
    swapped = (low * n + high) * 4 + r
    wanted = jnp.where(c == 0, swapped, rows)
    return jnp.where(cols == wanted, 1.0, 0.0).astype(BF)


def exchange(
    n,
    nx,
    total,
    normed_h,
    key_h,
    value_h,
    basis_ref,
    mk_ref,
    mv_ref,
    fk_ref,
    sk_ref,
    fv_ref,
    sv_ref,
    basis_out,
    m_out,
    d_out,
    nf_out,
    ns_out,
    normed_v,
    cot_v,
    cot_t,
    g_high,
    g_low,
    halves,
    moments,
    f32_first,
    f32_second,
    rs_send,
    rs_recv,
    ar_recv,
    sq1,
    sq2,
    local_sem,
    b1s,
    b1r,
    b2s,
    b2r,
    dds,
    ddr,
    m1s,
    m1r,
    m2s,
    m2r,
    fms,
    fmr,
    rss,
    rsr,
    ars,
    arr,
    q1s,
    q1r,
    q2s,
    q2r,
    ags,
    agr,
):
    z, y, x, c = (lax.axis_index(name) for name in AXES)
    kc = mk_ref.shape[1]
    rank = basis_ref.shape[1]
    a = y * (1 - c) + z * c
    b = z * (1 - c) + y * c
    t = x * 2 + c
    nt = nx * 2

    def first(d):
        return (lax.rem(z + d * c, n), lax.rem(y + d * (1 - c), n), x, c)

    def second(d):
        return (lax.rem(z + d * (1 - c), n), lax.rem(y + d * c, n), x, c)

    def across(d):
        other = lax.rem(t + d, nt)
        return (z, y, other // 2, lax.rem(other, 2))

    partner = (z, y, x, 1 - c)
    started = []

    def send(src, dst, send_sem, recv_sem, device):
        copy = pltpu.make_async_remote_copy(
            src_ref=src,
            dst_ref=dst,
            send_sem=send_sem,
            recv_sem=recv_sem,
            device_id=device,
            device_id_type=MESH,
        )
        copy.start()
        started.append(copy)
        return copy

    locals_ = [
        pltpu.make_async_copy(normed_h, normed_v, local_sem.at[0]),
        pltpu.make_async_copy(key_h, cot_v.at[:, pl.ds(0, kc)], local_sem.at[1]),
        pltpu.make_async_copy(value_h, cot_v.at[:, pl.ds(kc, value_h.shape[1])], local_sem.at[2]),
    ]
    for copy in locals_:
        copy.start()

    barrier = pltpu.get_barrier_semaphore()
    order = sorted(range(1, n), key=lambda d: -min(d, n - d))
    order_t = range(1, nt)
    for d in range(1, n):
        pl.semaphore_signal(barrier, inc=1, device_id=first(d), device_id_type=MESH)
        pl.semaphore_signal(barrier, inc=1, device_id=second(d), device_id_type=MESH)
    for d in order_t:
        pl.semaphore_signal(barrier, inc=1, device_id=across(d), device_id_type=MESH)

    half = basis_ref.shape[0] // 2
    mine = basis_ref.at[pl.ds(pl.multiple_of(c * half, half), half)]
    halves[c, b, a] = mine[...]
    m_out[b, a, :, :kc] = mk_ref[...].astype(BF)
    m_out[b, a, :, kc:] = mv_ref[...].astype(BF)
    moments[b, 0:4, :kc] = fk_ref[...]
    moments[b, 0:4, kc:] = fv_ref[...]
    moments[b, 4:8, :kc] = sk_ref[...]
    moments[b, 4:8, kc:] = sv_ref[...]
    pl.semaphore_wait(barrier, 2 * (n - 1) + nt - 1)

    b1 = [send(mine, halves.at[c, b, a], b1s.at[d], b1r.at[d], first(d)) for d in order]
    fm = [send(moments.at[b], moments.at[b], fms.at[d], fmr.at[d], second(d)) for d in order]
    m1 = [send(m_out.at[b, a], m_out.at[b, a], m1s.at[d], m1r.at[d], first(d)) for d in order]

    for copy in locals_:
        copy.wait()
    cot_t[...] = cot_v[...].astype(F32).T.astype(BF)
    wide = normed_v.shape[1]
    step = min(256, wide)

    @pl.loop(0, wide // step)
    def _(i):
        cols = pl.ds(pl.multiple_of(i * step, step), step)
        g = jnp.dot(cot_t[...], normed_v[:, cols], preferred_element_type=F32)
        high = g.astype(BF)
        g_high[:, cols] = high
        g_low[:, cols] = (g - high.astype(F32)).astype(BF)

    for copy in b1:
        copy.wait_recv()
    b2 = [send(halves.at[c, b], halves.at[c, b], b2s.at[d], b2r.at[d], second(d)) for d in order]
    dd = [send(halves.at[c, b], halves.at[c, b], dds.at[0], ddr.at[0], partner)]

    def ring(step, way, part):
        block = lax.rem(b - way * step + n, n)
        where = m_out.at[block] if part is None else m_out.at[block, pl.ds(part * (n // 2), n // 2)]
        k = 2 * step + (0 if way > 0 else 1)
        return send(where, where, m2s.at[k], m2r.at[k], second(way % n))

    def both_ways(step):
        last = step == n // 2 - 1
        return [ring(step, 1, 0 if last else None), ring(step, -1, 1 if last else None)]

    for copy in m1:
        copy.wait_recv()
    m2 = both_ways(0)
    for d, copy in zip(order, b2):
        copy.wait_recv()
        block = halves.at[c, lax.rem(b - d + n, n)]
        dd.append(send(block, block, dds.at[d], ddr.at[d], partner))
    for copy in fm:
        copy.wait_recv()
    for k in range(n):
        f32_first[4 * k : 4 * k + 4, :] = moments[k, 0:4, :]
        f32_second[4 * k : 4 * k + 4, :] = moments[k, 4:8, :]
    perm = permutation(n, c, rank)
    for copy in dd:
        copy.wait_recv()
    for zz in range(n):
        for yy in range(n):
            row = (zz * n + yy) * 2 * half
            basis_out[row : row + half, :] = halves[0, zz, yy]
            basis_out[row + half : row + 2 * half, :] = halves[1, yy, zz]
    low_t = jnp.dot(g_high[...], basis_out[...], preferred_element_type=F32)
    low_t = low_t + jnp.dot(g_low[...], basis_out[...], preferred_element_type=F32)
    flat = lax.dot_general(
        perm, low_t.astype(BF), (((1,), (1,)), ((), ())), preferred_element_type=F32
    ).astype(BF)
    lines = 4 * n
    for k in range(n):
        rs_send[k] = flat[k * lines : (k + 1) * lines, :]
    rs_recv[a] = rs_send[a]
    rs = [
        send(rs_send.at[lax.rem(a + d, n)], rs_recv.at[a], rss.at[d], rsr.at[d], first(d))
        for d in order
    ]

    def forward(held, step):
        for copy in held:
            copy.wait_recv()
        return both_ways(step)

    held = m2
    if n // 2 > 1:
        held = forward(held, 1)
    for copy in rs:
        copy.wait_recv()
    ar_recv[b] = functools.reduce(jnp.add, [rs_recv[k].astype(F32) for k in range(n)])
    ar = [send(ar_recv.at[b], ar_recv.at[b], ars.at[d], arr.at[d], second(d)) for d in order]
    if n // 2 > 2:
        held = forward(held, 2)
    for copy in ar:
        copy.wait_recv()
    low = functools.reduce(jnp.add, [ar_recv[k] for k in range(n)])
    squares = low * low
    squares = functools.reduce(
        jnp.add, [squares[8 * k : 8 * k + 8, :] for k in range(lines // 8)]
    )
    squares = functools.reduce(
        jnp.add, [squares[:, 128 * k : 128 * k + 128] for k in range(squares.shape[1] // 128)]
    )
    sq1[a] = squares
    q1 = [send(sq1.at[a], sq1.at[a], q1s.at[d], q1r.at[d], first(d)) for d in order]
    if n // 2 > 3:
        held = forward(held, 3)
    for copy in q1:
        copy.wait_recv()
    sq2[t] = functools.reduce(jnp.add, [sq1[k] for k in range(n)])
    q2 = [send(sq2.at[t], sq2.at[t], q2s.at[d], q2r.at[d], across(d)) for d in order_t]
    for copy in q2:
        copy.wait_recv()
    squares = functools.reduce(jnp.add, [sq2[k] for k in range(nt)])
    squares = jnp.sum(jnp.sum(squares, axis=1, keepdims=True), axis=0, keepdims=True)
    grad_scale = 1.0 / jnp.sqrt(squares / total + norm_eps)
    scaled = low * grad_scale
    new_first = beta_first * f32_first[...] + (1.0 - beta_first) * scaled
    new_second = beta_second * f32_second[...] + (1.0 - beta_second) * scaled * scaled
    d_out[a] = (new_first / (jnp.sqrt(new_second) + epsilon)).astype(BF)
    ag = [send(d_out.at[a], d_out.at[a], ags.at[d], agr.at[d], first(d)) for d in order]
    nf_out[...] = new_first
    ns_out[...] = new_second
    for copy in held:
        copy.wait_recv()
    for copy in ag:
        copy.wait_recv()
    for copy in started:
        copy.wait_send()


def finish(
    n,
    basis_all,
    m_all,
    d_all,
    nf_all,
    ns_all,
    basis_ref,
    mk_ref,
    mv_ref,
    step_key,
    step_value,
    new_key,
    new_value,
    copy_key,
    copy_value,
    nfk,
    nsk,
    nfv,
    nsv,
    directions,
):
    c = lax.axis_index("c")
    b = lax.axis_index("z") * (1 - c) + lax.axis_index("y") * c
    kc = mk_ref.shape[1]
    i = pl.program_id(0)
    rank = basis_ref.shape[1]

    @pl.when(i == 0)
    def _():
        flat = d_all[...].reshape(rank, d_all.shape[2])
        directions[...] = jnp.dot(
            permutation(n, c, rank), flat, preferred_element_type=F32
        ).astype(BF)
        own = jnp.dot(basis_ref[...], directions[...], preferred_element_type=F32)
        step_key[...] = own[:, :kc]
        step_value[...] = own[:, kc:]
        new_key[...] = mk_ref[...] - learn_rate * own[:, :kc]
        new_value[...] = mv_ref[...] - learn_rate * own[:, kc:]
        for src, key_out, value_out in ((nf_all, nfk, nfv), (ns_all, nsk, nsv)):
            rows = src[0:4, :]
            for k in range(1, n):
                rows = jnp.where(b == k, src[4 * k : 4 * k + 4, :], rows)
            key_out[...] = rows[:, :kc]
            value_out[...] = rows[:, kc:]

    part = jnp.dot(basis_all[...], directions[...], preferred_element_type=F32)
    height = m_all.shape[2]
    for k in range(copy_key.shape[0] // height):
        block = i * (copy_key.shape[0] // height) + k
        high, low = block // n, lax.rem(block, n)
        master = m_all[high * (1 - c) + low * c, low * (1 - c) + high * c].astype(F32)
        rows = slice(k * height, (k + 1) * height)
        out = (master - learn_rate * part[rows, :]).astype(BF)
        copy_key[rows, :] = out[:, :kc]
        copy_value[rows, :] = out[:, kc:]


def on_device(n, nx, normed, key_cot, value_cot, basis, mk, mv, fk, sk, fv, sv):
    kc, vc = key_cot.shape[1], value_cot.shape[1]
    cols = kc + vc
    rows, rank = basis.shape
    tokens, width = normed.shape
    total = rank * cols * nx * 2
    anywhere = pl.BlockSpec(memory_space=pl.ANY)
    vmem = pl.BlockSpec(memory_space=VMEM)
    shape = jax.ShapeDtypeStruct
    lines = 4 * n
    basis_all, m_all, d_all, nf_all, ns_all = pl.pallas_call(
        functools.partial(exchange, n, nx, total),
        name="exchange",
        out_shape=(
            shape((width, rank), BF),
            shape((n, n, rows, cols), BF),
            shape((n, lines, cols), BF),
            shape((lines, cols), F32),
            shape((lines, cols), F32),
        ),
        in_specs=[anywhere] * 3 + [vmem] * 7,
        out_specs=(vmem,) * 5,
        scratch_shapes=[
            VMEM((tokens, width), BF),
            VMEM((tokens, cols), BF),
            VMEM((cols, tokens), BF),
            VMEM((cols, width), BF),
            VMEM((cols, width), BF),
            VMEM((2, n, n, rows // 2, rank), BF),
            VMEM((n, 8, cols), F32),
            VMEM((lines, cols), F32),
            VMEM((lines, cols), F32),
            VMEM((n, lines, cols), BF),
            VMEM((n, lines, cols), BF),
            VMEM((n, lines, cols), F32),
            VMEM((n, 8, 128), F32),
            VMEM((nx * 2, 8, 128), F32),
            DMA((3,)),
        ]
        + [DMA((n,))] * 18
        + [DMA((nx * 2,))] * 2
        + [DMA((n,))] * 2,
        compiler_params=pltpu.CompilerParams(
            collective_id=0, has_side_effects=True, vmem_limit_bytes=48 * 2**20
        ),
    )(normed, key_cot, value_cot, basis, mk, mv, fk, sk, fv, sv)
    steps = 4
    tall = width // steps

    def whole(*dims):
        return pl.BlockSpec(dims, lambda i: (0,) * len(dims))

    return pl.pallas_call(
        functools.partial(finish, n),
        name="finish",
        grid=(steps,),
        out_shape=(
            shape((rows, kc), F32),
            shape((rows, vc), F32),
            shape((rows, kc), F32),
            shape((rows, vc), F32),
            shape((width, kc), BF),
            shape((width, vc), BF),
            shape((4, kc), F32),
            shape((4, kc), F32),
            shape((4, vc), F32),
            shape((4, vc), F32),
        ),
        in_specs=[
            pl.BlockSpec((tall, rank), lambda i: (i, 0)),
            whole(n, n, rows, cols),
            whole(n, lines, cols),
            whole(lines, cols),
            whole(lines, cols),
            whole(rows, rank),
            whole(rows, kc),
            whole(rows, vc),
        ],
        out_specs=(
            whole(rows, kc),
            whole(rows, vc),
            whole(rows, kc),
            whole(rows, vc),
            pl.BlockSpec((tall, kc), lambda i: (i, 0)),
            pl.BlockSpec((tall, vc), lambda i: (i, 0)),
            whole(4, kc),
            whole(4, kc),
            whole(4, vc),
            whole(4, vc),
        ),
        scratch_shapes=[VMEM((rank, cols), BF)],
    )(basis_all, m_all, d_all, nf_all, ns_all, basis, mk, mv)


def solution(mesh):
    n = 8
    nx = mesh.devices.size // (2 * n * n)
    torus = Mesh(mesh.devices.reshape(n, n, nx, 2), AXES)
    split = P(FS, TP)
    return jax.shard_map(
        functools.partial(on_device, n, nx),
        mesh=torus,
        in_specs=(P(FS, None), split, split, P(FS, None)) + (split,) * 6,
        out_specs=(split,) * 4 + (P(None, TP),) * 2 + (split,) * 4,
        check_vma=False,
    )
```

```python
import functools

import jax
import jax.numpy as jnp
from jax import lax
from jax.experimental import pallas as pl
from jax.experimental.pallas import tpu as pltpu
from jax.sharding import Mesh
from jax.sharding import PartitionSpec as P

AXES = ("z", "y", "x", "c")
FS = ("z", "y")
TP = ("x", "c")
MESH = pl.DeviceIdType.MESH
VMEM = pltpu.VMEM
DMA = pltpu.SemaphoreType.DMA
BF = jnp.bfloat16
F32 = jnp.float32

learn_rate = 0.05
beta_first = 0.9
beta_second = 0.9
epsilon = 1e-08
norm_eps = 1e-06
PARTS = 4


def permutation(n, c, rank):
    rows = lax.broadcasted_iota(jnp.int32, (rank, rank), 0)
    cols = lax.broadcasted_iota(jnp.int32, (rank, rank), 1)
    r = rows % 4
    low = (rows // 4) % n
    high = rows // (4 * n)
    swapped = (low * n + high) * 4 + r
    wanted = jnp.where(c == 0, swapped, rows)
    return jnp.where(cols == wanted, 1.0, 0.0).astype(BF)


def exchange(
    n,
    nx,
    total,
    normed_h,
    key_h,
    value_h,
    basis_h,
    mk_h,
    mv_h,
    fk_h,
    sk_h,
    fv_h,
    sv_h,
    basis_out,
    m_out,
    d_out,
    nf_out,
    ns_out,
    master_out,
    normed_v,
    cot_v,
    cot_t,
    g_high,
    g_low,
    halves,
    moments,
    fk_ref,
    sk_ref,
    fv_ref,
    sv_ref,
    f32_first,
    f32_second,
    rs_send,
    rs_recv,
    ar_recv,
    sq1,
    sq2,
    local_sem,
    b1s,
    b1r,
    b2s,
    b2r,
    dds,
    ddr,
    m1s,
    m1r,
    m2s,
    m2r,
    fms,
    fmr,
    rss,
    rsr,
    ars,
    arr,
    q1s,
    q1r,
    q2s,
    q2r,
    ags,
    agr,
):
    z, y, x, c = (lax.axis_index(name) for name in AXES)
    kc, vc = key_h.shape[1], value_h.shape[1]
    rank = basis_h.shape[1]
    a = y * (1 - c) + z * c
    b = z * (1 - c) + y * c
    t = x * 2 + c
    nt = nx * 2

    def first(d):
        return (lax.rem(z + d * c, n), lax.rem(y + d * (1 - c), n), x, c)

    def second(d):
        return (lax.rem(z + d * (1 - c), n), lax.rem(y + d * c, n), x, c)

    def across(d):
        other = lax.rem(t + d, nt)
        return (z, y, other // 2, lax.rem(other, 2))

    partner = (z, y, x, 1 - c)
    started = []

    def send(src, dst, send_sem, recv_sem, device):
        copy = pltpu.make_async_remote_copy(
            src_ref=src,
            dst_ref=dst,
            send_sem=send_sem,
            recv_sem=recv_sem,
            device_id=device,
            device_id_type=MESH,
        )
        copy.start()
        started.append(copy)
        return copy

    half = basis_h.shape[0] // 2
    mine = halves.at[c, b, a]
    small, large = [
        [pltpu.make_async_copy(src, dst, local_sem.at[k]) for k, src, dst in pairs]
        for pairs in (
            (
                (0, basis_h.at[pl.ds(pl.multiple_of(c * half, half), half)], mine),
                (1, fk_h, fk_ref),
                (2, sk_h, sk_ref),
                (3, fv_h, fv_ref),
                (4, sv_h, sv_ref),
                (5, mk_h, master_out.at[:, pl.ds(0, kc)]),
                (6, mv_h, master_out.at[:, pl.ds(kc, vc)]),
            ),
            (
                (7, key_h, cot_v.at[:, pl.ds(0, kc)]),
                (8, value_h, cot_v.at[:, pl.ds(kc, vc)]),
                (9, normed_h, normed_v),
            ),
        )
    ]
    for copy in small + large:
        copy.start()

    barrier = pltpu.get_barrier_semaphore()
    order = sorted(range(1, n), key=lambda d: -min(d, n - d))
    order_t = range(1, nt)
    for d in range(1, n):
        pl.semaphore_signal(barrier, inc=1, device_id=first(d), device_id_type=MESH)
        pl.semaphore_signal(barrier, inc=1, device_id=second(d), device_id_type=MESH)
    for d in order_t:
        pl.semaphore_signal(barrier, inc=1, device_id=across(d), device_id_type=MESH)

    for copy in small:
        copy.wait()
    m_out[b, a] = master_out[...].astype(BF)
    moments[b, 0:4, :kc] = fk_ref[...]
    moments[b, 0:4, kc:] = fv_ref[...]
    moments[b, 4:8, :kc] = sk_ref[...]
    moments[b, 4:8, kc:] = sv_ref[...]
    pl.semaphore_wait(barrier, 2 * (n - 1) + nt - 1)

    b1 = [send(mine, halves.at[c, b, a], b1s.at[d], b1r.at[d], first(d)) for d in order]
    fm = [send(moments.at[b], moments.at[b], fms.at[d], fmr.at[d], second(d)) for d in order]
    m1 = [send(m_out.at[b, a], m_out.at[b, a], m1s.at[d], m1r.at[d], first(d)) for d in order]

    for copy in large:
        copy.wait()
    cot_t[...] = cot_v[...].astype(F32).T.astype(BF)
    wide = normed_v.shape[1]
    step = min(256, wide)

    @pl.loop(0, wide // step)
    def _(i):
        cols = pl.ds(pl.multiple_of(i * step, step), step)
        g = jnp.dot(cot_t[...], normed_v[:, cols], preferred_element_type=F32)
        high = g.astype(BF)
        g_high[:, cols] = high
        g_low[:, cols] = (g - high.astype(F32)).astype(BF)

    for copy in b1:
        copy.wait_recv()
    b2 = [send(halves.at[c, b], halves.at[c, b], b2s.at[d], b2r.at[d], second(d)) for d in order]
    dd = [send(halves.at[c, b], halves.at[c, b], dds.at[0], ddr.at[0], partner)]

    def ring(step, way, part):
        block = lax.rem(b - way * step + n, n)
        where = m_out.at[block] if part is None else m_out.at[block, pl.ds(part * (n // 2), n // 2)]
        k = 2 * step + (0 if way > 0 else 1)
        return send(where, where, m2s.at[k], m2r.at[k], second(way % n))

    def both_ways(step):
        last = step == n // 2 - 1
        return [ring(step, 1, 0 if last else None), ring(step, -1, 1 if last else None)]

    for copy in m1:
        copy.wait_recv()
    m2 = both_ways(0)
    for d, copy in zip(order, b2):
        copy.wait_recv()
        block = halves.at[c, lax.rem(b - d + n, n)]
        dd.append(send(block, block, dds.at[d], ddr.at[d], partner))
    for copy in fm:
        copy.wait_recv()
    for k in range(n):
        f32_first[4 * k : 4 * k + 4, :] = moments[k, 0:4, :]
        f32_second[4 * k : 4 * k + 4, :] = moments[k, 4:8, :]
    perm = permutation(n, c, rank)
    for copy in dd:
        copy.wait_recv()
    for zz in range(n):
        for yy in range(n):
            row = (zz * n + yy) * 2 * half
            basis_out[row : row + half, :] = halves[0, zz, yy]
            basis_out[row + half : row + 2 * half, :] = halves[1, yy, zz]
    low_t = jnp.dot(g_high[...], basis_out[...], preferred_element_type=F32)
    low_t = low_t + jnp.dot(g_low[...], basis_out[...], preferred_element_type=F32)
    flat = lax.dot_general(
        perm, low_t.astype(BF), (((1,), (1,)), ((), ())), preferred_element_type=F32
    ).astype(BF)
    lines = 4 * n
    for k in range(n):
        rs_send[k] = flat[k * lines : (k + 1) * lines, :]
    rs_recv[a] = rs_send[a]
    rs = [
        send(rs_send.at[lax.rem(a + d, n)], rs_recv.at[a], rss.at[d], rsr.at[d], first(d))
        for d in order
    ]

    def forward(held, step):
        for copy in held:
            copy.wait_recv()
        return both_ways(step)

    held = m2
    if n // 2 > 1:
        held = forward(held, 1)
    for copy in rs:
        copy.wait_recv()
    ar_recv[b] = functools.reduce(jnp.add, [rs_recv[k].astype(F32) for k in range(n)])
    ar = [send(ar_recv.at[b], ar_recv.at[b], ars.at[d], arr.at[d], second(d)) for d in order]
    if n // 2 > 2:
        held = forward(held, 2)
    for copy in ar:
        copy.wait_recv()
    low = functools.reduce(jnp.add, [ar_recv[k] for k in range(n)])
    squares = low * low
    squares = functools.reduce(
        jnp.add, [squares[8 * k : 8 * k + 8, :] for k in range(lines // 8)]
    )
    squares = functools.reduce(
        jnp.add, [squares[:, 128 * k : 128 * k + 128] for k in range(squares.shape[1] // 128)]
    )
    sq1[a] = squares
    q1 = [send(sq1.at[a], sq1.at[a], q1s.at[d], q1r.at[d], first(d)) for d in order]
    if n // 2 > 3:
        held = forward(held, 3)
    for copy in q1:
        copy.wait_recv()
    sq2[t] = functools.reduce(jnp.add, [sq1[k] for k in range(n)])
    q2 = [send(sq2.at[t], sq2.at[t], q2s.at[d], q2r.at[d], across(d)) for d in order_t]
    for copy in q2:
        copy.wait_recv()
    squares = functools.reduce(jnp.add, [sq2[k] for k in range(nt)])
    squares = jnp.sum(jnp.sum(squares, axis=1, keepdims=True), axis=0, keepdims=True)
    grad_scale = 1.0 / jnp.sqrt(squares / total + norm_eps)
    scaled = low * grad_scale
    new_first = beta_first * f32_first[...] + (1.0 - beta_first) * scaled
    new_second = beta_second * f32_second[...] + (1.0 - beta_second) * scaled * scaled
    d_out[a] = (new_first / (jnp.sqrt(new_second) + epsilon)).astype(BF)
    ag = [send(d_out.at[a], d_out.at[a], ags.at[d], agr.at[d], first(d)) for d in order]
    for out, new in ((nf_out, new_first), (ns_out, new_second)):
        rows = new[0:4, :]
        for k in range(1, n):
            rows = jnp.where(b == k, new[4 * k : 4 * k + 4, :], rows)
        out[...] = rows
    for copy in held:
        copy.wait_recv()
    for copy in ag:
        copy.wait_recv()
    for copy in started:
        copy.wait_send()


def finish(
    n,
    basis_all,
    m_all,
    d_all,
    nf_all,
    ns_all,
    master_own,
    step_key,
    step_value,
    new_key,
    new_value,
    copy_key,
    copy_value,
    nfk,
    nsk,
    nfv,
    nsv,
    directions,
    copies,
    step_v,
    new_v,
    sems,
):
    z, y, c = (lax.axis_index(name) for name in ("z", "y", "c"))
    kc, vc = copy_key.shape[1], copy_value.shape[1]
    rank = basis_all.shape[1]
    height = m_all.shape[2]
    tall = basis_all.shape[0] // PARTS
    started = []

    def put(src, key_dst, value_dst):
        for dst, cols in ((key_dst, pl.ds(0, kc)), (value_dst, pl.ds(kc, vc))):
            copy = pltpu.make_async_copy(src.at[:, cols], dst, sems.at[len(started)])
            copy.start()
            started.append(copy)

    put(nf_all, nfk, nfv)
    put(ns_all, nsk, nsv)
    flat = d_all[...].reshape(rank, d_all.shape[2])
    directions[...] = jnp.dot(permutation(n, c, rank), flat, preferred_element_type=F32).astype(BF)
    for i in range(PARTS):
        rows = pl.ds(i * tall, tall)
        part = jnp.dot(basis_all[rows, :], directions[...], preferred_element_type=F32)
        for k in range(tall // height):
            block = i * (tall // height) + k
            high, low = block // n, block % n
            master = m_all[high * (1 - c) + low * c, low * (1 - c) + high * c].astype(F32)
            moved = master - learn_rate * part[k * height : (k + 1) * height, :]
            copies[block * height : (block + 1) * height, :] = moved.astype(BF)
        put(copies.at[rows], copy_key.at[rows], copy_value.at[rows])
    mine = pl.ds(pl.multiple_of((z * n + y) * height, height), height)
    own = jnp.dot(basis_all[mine, :], directions[...], preferred_element_type=F32)
    step_v[...] = own
    new_v[...] = master_own[...] - learn_rate * own
    put(step_v, step_key, step_value)
    put(new_v, new_key, new_value)
    for copy in started:
        copy.wait()


def on_device(n, nx, *arrays):
    normed, key_cot, value_cot, basis = arrays[:4]
    kc, vc = key_cot.shape[1], value_cot.shape[1]
    cols = kc + vc
    rows, rank = basis.shape
    tokens, width = normed.shape
    total = rank * cols * nx * 2
    hbm = pl.BlockSpec(memory_space=pltpu.HBM)
    vmem = pl.BlockSpec(memory_space=VMEM)
    shape = jax.ShapeDtypeStruct
    lines = 4 * n
    gathered = pl.pallas_call(
        functools.partial(exchange, n, nx, total),
        name="exchange",
        out_shape=(
            shape((width, rank), BF),
            shape((n, n, rows, cols), BF),
            shape((n, lines, cols), BF),
            shape((4, cols), F32),
            shape((4, cols), F32),
            shape((rows, cols), F32),
        ),
        in_specs=[hbm] * 10,
        out_specs=(vmem,) * 6,
        scratch_shapes=[
            VMEM((tokens, width), BF),
            VMEM((tokens, cols), BF),
            VMEM((cols, tokens), BF),
            VMEM((cols, width), BF),
            VMEM((cols, width), BF),
            VMEM((2, n, n, rows // 2, rank), BF),
            VMEM((n, 8, cols), F32),
            VMEM((4, kc), F32),
            VMEM((4, kc), F32),
            VMEM((4, vc), F32),
            VMEM((4, vc), F32),
            VMEM((lines, cols), F32),
            VMEM((lines, cols), F32),
            VMEM((n, lines, cols), BF),
            VMEM((n, lines, cols), BF),
            VMEM((n, lines, cols), F32),
            VMEM((n, 8, 128), F32),
            VMEM((nx * 2, 8, 128), F32),
            DMA((10,)),
        ]
        + [DMA((n,))] * 18
        + [DMA((nx * 2,))] * 2
        + [DMA((n,))] * 2,
        compiler_params=pltpu.CompilerParams(
            collective_id=0, has_side_effects=True, vmem_limit_bytes=40 * 2**20
        ),
    )(*(pltpu.with_memory_space_constraint(array, pltpu.HBM) for array in arrays))
    return pl.pallas_call(
        functools.partial(finish, n),
        name="finish",
        out_shape=(
            shape((rows, kc), F32),
            shape((rows, vc), F32),
            shape((rows, kc), F32),
            shape((rows, vc), F32),
            shape((width, kc), BF),
            shape((width, vc), BF),
            shape((4, kc), F32),
            shape((4, kc), F32),
            shape((4, vc), F32),
            shape((4, vc), F32),
        ),
        in_specs=[vmem] * 6,
        out_specs=(hbm,) * 10,
        scratch_shapes=[
            VMEM((rank, cols), BF),
            VMEM((width, cols), BF),
            VMEM((rows, cols), F32),
            VMEM((rows, cols), F32),
            DMA((2 * (PARTS + 4),)),
        ],
        compiler_params=pltpu.CompilerParams(vmem_limit_bytes=24 * 2**20),
    )(*gathered)


def solution(mesh):
    n = 8
    nx = mesh.devices.size // (2 * n * n)
    torus = Mesh(mesh.devices.reshape(n, n, nx, 2), AXES)
    split = P(FS, TP)
    return jax.shard_map(
        functools.partial(on_device, n, nx),
        mesh=torus,
        in_specs=(P(FS, None), split, split, P(FS, None)) + (split,) * 6,
        out_specs=(split,) * 4 + (P(None, TP),) * 2 + (split,) * 4,
        check_vma=False,
    )
```

```python
import functools

import jax
import jax.numpy as jnp
from jax import lax
from jax.experimental import pallas as pl
from jax.experimental.pallas import tpu as pltpu
from jax.sharding import Mesh
from jax.sharding import PartitionSpec as P

AXES = ("z", "y", "x", "c")
FS = ("z", "y")
TP = ("x", "c")
MESH = pl.DeviceIdType.MESH
VMEM = pltpu.VMEM
DMA = pltpu.SemaphoreType.DMA
BF = jnp.bfloat16
F32 = jnp.float32

learn_rate = 0.05
beta_first = 0.9
beta_second = 0.9
epsilon = 1e-08
norm_eps = 1e-06
PARTS = 4


def permutation(n, c, rank):
    rows = lax.broadcasted_iota(jnp.int32, (rank, rank), 0)
    cols = lax.broadcasted_iota(jnp.int32, (rank, rank), 1)
    r = rows % 4
    low = (rows // 4) % n
    high = rows // (4 * n)
    swapped = (low * n + high) * 4 + r
    wanted = jnp.where(c == 0, swapped, rows)
    return jnp.where(cols == wanted, 1.0, 0.0).astype(BF)


def exchange(
    n,
    nx,
    total,
    normed_h,
    key_h,
    value_h,
    basis_h,
    mk_h,
    mv_h,
    fk_h,
    sk_h,
    fv_h,
    sv_h,
    basis_out,
    m_out,
    d_out,
    nf_out,
    ns_out,
    master_out,
    normed_v,
    cot_v,
    cot_t,
    g_high,
    g_low,
    halves,
    moments,
    fk_ref,
    sk_ref,
    fv_ref,
    sv_ref,
    f32_first,
    f32_second,
    rs_send,
    rs_recv,
    ar_recv,
    sq1,
    sq2,
    local_sem,
    b1s,
    b1r,
    b2s,
    b2r,
    dds,
    ddr,
    m1s,
    m1r,
    m2s,
    m2r,
    fms,
    fmr,
    rss,
    rsr,
    ars,
    arr,
    q1s,
    q1r,
    q2s,
    q2r,
    ags,
    agr,
):
    z, y, x, c = (lax.axis_index(name) for name in AXES)
    kc, vc = key_h.shape[1], value_h.shape[1]
    rank = basis_h.shape[1]
    a = y * (1 - c) + z * c
    b = z * (1 - c) + y * c
    t = x * 2 + c
    nt = nx * 2

    def first(d):
        return (lax.rem(z + d * c, n), lax.rem(y + d * (1 - c), n), x, c)

    def second(d):
        return (lax.rem(z + d * (1 - c), n), lax.rem(y + d * c, n), x, c)

    def across(d):
        other = lax.rem(t + d, nt)
        return (z, y, other // 2, lax.rem(other, 2))

    partner = (z, y, x, 1 - c)
    started = []

    def send(src, dst, send_sem, recv_sem, device):
        copy = pltpu.make_async_remote_copy(
            src_ref=src,
            dst_ref=dst,
            send_sem=send_sem,
            recv_sem=recv_sem,
            device_id=device,
            device_id_type=MESH,
        )
        copy.start()
        started.append(copy)
        return copy

    half = basis_h.shape[0] // 2
    mine = halves.at[c, b, a]
    small, large = [
        [pltpu.make_async_copy(src, dst, local_sem.at[k]) for k, src, dst in pairs]
        for pairs in (
            (
                (0, basis_h.at[pl.ds(pl.multiple_of(c * half, half), half)], mine),
                (1, fk_h, fk_ref),
                (2, sk_h, sk_ref),
                (3, fv_h, fv_ref),
                (4, sv_h, sv_ref),
                (5, mk_h, master_out.at[:, pl.ds(0, kc)]),
                (6, mv_h, master_out.at[:, pl.ds(kc, vc)]),
            ),
            (
                (7, key_h, cot_v.at[:, pl.ds(0, kc)]),
                (8, value_h, cot_v.at[:, pl.ds(kc, vc)]),
                (9, normed_h, normed_v),
            ),
        )
    ]
    for copy in small + large:
        copy.start()

    barrier = pltpu.get_barrier_semaphore()
    order = sorted(range(1, n), key=lambda d: -min(d, n - d))
    order_t = range(1, nt)
    for d in range(1, n):
        pl.semaphore_signal(barrier, inc=1, device_id=first(d), device_id_type=MESH)
        pl.semaphore_signal(barrier, inc=1, device_id=second(d), device_id_type=MESH)
    for d in order_t:
        pl.semaphore_signal(barrier, inc=1, device_id=across(d), device_id_type=MESH)

    for copy in small:
        copy.wait()
    m_out[b, a] = master_out[...].astype(BF)
    moments[b, 0:4, :kc] = fk_ref[...]
    moments[b, 0:4, kc:] = fv_ref[...]
    moments[b, 4:8, :kc] = sk_ref[...]
    moments[b, 4:8, kc:] = sv_ref[...]
    pl.semaphore_wait(barrier, 2 * (n - 1) + nt - 1)

    b1 = [send(mine, halves.at[c, b, a], b1s.at[d], b1r.at[d], first(d)) for d in order]

    for copy in b1:
        copy.wait_recv()
    b2 = [send(halves.at[c, b], halves.at[c, b], b2s.at[d], b2r.at[d], second(d)) for d in order]
    dd = [send(halves.at[c, b], halves.at[c, b], dds.at[0], ddr.at[0], partner)]
    fm = [send(moments.at[b], moments.at[b], fms.at[d], fmr.at[d], second(d)) for d in order]
    m1 = [send(m_out.at[b, a], m_out.at[b, a], m1s.at[d], m1r.at[d], first(d)) for d in order]

    for copy in large:
        copy.wait()
    cot_t[...] = cot_v[...].astype(F32).T.astype(BF)
    wide = normed_v.shape[1]
    step = min(256, wide)

    @pl.loop(0, wide // step)
    def _(i):
        cols = pl.ds(pl.multiple_of(i * step, step), step)
        g = jnp.dot(cot_t[...], normed_v[:, cols], preferred_element_type=F32)
        high = g.astype(BF)
        g_high[:, cols] = high
        g_low[:, cols] = (g - high.astype(F32)).astype(BF)

    def ring(step, way, part):
        block = lax.rem(b - way * step + n, n)
        where = m_out.at[block] if part is None else m_out.at[block, pl.ds(part * (n // 2), n // 2)]
        k = 2 * step + (0 if way > 0 else 1)
        return send(where, where, m2s.at[k], m2r.at[k], second(way % n))

    def both_ways(step):
        last = step == n // 2 - 1
        return [ring(step, 1, 0 if last else None), ring(step, -1, 1 if last else None)]

    for d, copy in zip(order, b2):
        copy.wait_recv()
        block = halves.at[c, lax.rem(b - d + n, n)]
        dd.append(send(block, block, dds.at[d], ddr.at[d], partner))
    perm = permutation(n, c, rank)
    for copy in dd:
        copy.wait_recv()
    for zz in range(n):
        for yy in range(n):
            row = (zz * n + yy) * 2 * half
            basis_out[row : row + half, :] = halves[0, zz, yy]
            basis_out[row + half : row + 2 * half, :] = halves[1, yy, zz]
    low_t = jnp.dot(g_high[...], basis_out[...], preferred_element_type=F32)
    low_t = low_t + jnp.dot(g_low[...], basis_out[...], preferred_element_type=F32)
    flat = lax.dot_general(
        perm, low_t.astype(BF), (((1,), (1,)), ((), ())), preferred_element_type=F32
    ).astype(BF)
    lines = 4 * n
    for k in range(n):
        rs_send[k] = flat[k * lines : (k + 1) * lines, :]
    rs_recv[a] = rs_send[a]
    rs = [
        send(rs_send.at[lax.rem(a + d, n)], rs_recv.at[a], rss.at[d], rsr.at[d], first(d))
        for d in order
    ]

    def forward(held, step):
        for copy in held:
            copy.wait_recv()
        return both_ways(step)

    held = forward(m1, 0)
    for copy in fm:
        copy.wait_recv()
    for k in range(n):
        f32_first[4 * k : 4 * k + 4, :] = moments[k, 0:4, :]
        f32_second[4 * k : 4 * k + 4, :] = moments[k, 4:8, :]
    for copy in rs:
        copy.wait_recv()
    ar_recv[b] = functools.reduce(jnp.add, [rs_recv[k].astype(F32) for k in range(n)]).astype(BF)
    ar = [send(ar_recv.at[b], ar_recv.at[b], ars.at[d], arr.at[d], second(d)) for d in order]
    if n // 2 > 1:
        held = forward(held, 1)
    for copy in ar:
        copy.wait_recv()
    low = functools.reduce(jnp.add, [ar_recv[k].astype(F32) for k in range(n)])
    squares = low * low
    squares = functools.reduce(
        jnp.add, [squares[8 * k : 8 * k + 8, :] for k in range(lines // 8)]
    )
    squares = functools.reduce(
        jnp.add, [squares[:, 128 * k : 128 * k + 128] for k in range(squares.shape[1] // 128)]
    )
    sq1[a] = squares
    q1 = [send(sq1.at[a], sq1.at[a], q1s.at[d], q1r.at[d], first(d)) for d in order]
    if n // 2 > 2:
        held = forward(held, 2)
    for copy in q1:
        copy.wait_recv()
    sq2[t] = functools.reduce(jnp.add, [sq1[k] for k in range(n)])
    q2 = [send(sq2.at[t], sq2.at[t], q2s.at[d], q2r.at[d], across(d)) for d in order_t]
    if n // 2 > 3:
        held = forward(held, 3)
    for copy in q2:
        copy.wait_recv()
    squares = functools.reduce(jnp.add, [sq2[k] for k in range(nt)])
    squares = jnp.sum(jnp.sum(squares, axis=1, keepdims=True), axis=0, keepdims=True)
    grad_scale = 1.0 / jnp.sqrt(squares / total + norm_eps)
    scaled = low * grad_scale
    new_first = beta_first * f32_first[...] + (1.0 - beta_first) * scaled
    new_second = beta_second * f32_second[...] + (1.0 - beta_second) * scaled * scaled
    d_out[a] = (new_first / (jnp.sqrt(new_second) + epsilon)).astype(BF)
    ag = [send(d_out.at[a], d_out.at[a], ags.at[d], agr.at[d], first(d)) for d in order]
    for out, new in ((nf_out, new_first), (ns_out, new_second)):
        rows = new[0:4, :]
        for k in range(1, n):
            rows = jnp.where(b == k, new[4 * k : 4 * k + 4, :], rows)
        out[...] = rows
    for copy in held:
        copy.wait_recv()
    for copy in ag:
        copy.wait_recv()
    for copy in started:
        copy.wait_send()


def finish(
    n,
    basis_all,
    m_all,
    d_all,
    nf_all,
    ns_all,
    master_own,
    step_key,
    step_value,
    new_key,
    new_value,
    copy_key,
    copy_value,
    nfk,
    nsk,
    nfv,
    nsv,
    directions,
    copies,
    step_v,
    new_v,
    sems,
):
    z, y, c = (lax.axis_index(name) for name in ("z", "y", "c"))
    kc, vc = copy_key.shape[1], copy_value.shape[1]
    rank = basis_all.shape[1]
    height = m_all.shape[2]
    tall = basis_all.shape[0] // PARTS
    started = []

    def put(src, key_dst, value_dst):
        for dst, cols in ((key_dst, pl.ds(0, kc)), (value_dst, pl.ds(kc, vc))):
            copy = pltpu.make_async_copy(src.at[:, cols], dst, sems.at[len(started)])
            copy.start()
            started.append(copy)

    put(nf_all, nfk, nfv)
    put(ns_all, nsk, nsv)
    flat = d_all[...].reshape(rank, d_all.shape[2])
    directions[...] = jnp.dot(permutation(n, c, rank), flat, preferred_element_type=F32).astype(BF)
    for i in range(PARTS):
        rows = pl.ds(i * tall, tall)
        part = jnp.dot(basis_all[rows, :], directions[...], preferred_element_type=F32)
        for k in range(tall // height):
            block = i * (tall // height) + k
            high, low = block // n, block % n
            master = m_all[high * (1 - c) + low * c, low * (1 - c) + high * c].astype(F32)
            moved = master - learn_rate * part[k * height : (k + 1) * height, :]
            copies[block * height : (block + 1) * height, :] = moved.astype(BF)
        put(copies.at[rows], copy_key.at[rows], copy_value.at[rows])
    mine = pl.ds(pl.multiple_of((z * n + y) * height, height), height)
    own = jnp.dot(basis_all[mine, :], directions[...], preferred_element_type=F32)
    step_v[...] = own
    new_v[...] = master_own[...] - learn_rate * own
    put(step_v, step_key, step_value)
    put(new_v, new_key, new_value)
    for copy in started:
        copy.wait()


def on_device(n, nx, *arrays):
    normed, key_cot, value_cot, basis = arrays[:4]
    kc, vc = key_cot.shape[1], value_cot.shape[1]
    cols = kc + vc
    rows, rank = basis.shape
    tokens, width = normed.shape
    total = rank * cols * nx * 2
    hbm = pl.BlockSpec(memory_space=pltpu.HBM)
    vmem = pl.BlockSpec(memory_space=VMEM)
    shape = jax.ShapeDtypeStruct
    lines = 4 * n
    gathered = pl.pallas_call(
        functools.partial(exchange, n, nx, total),
        name="exchange",
        out_shape=(
            shape((width, rank), BF),
            shape((n, n, rows, cols), BF),
            shape((n, lines, cols), BF),
            shape((4, cols), F32),
            shape((4, cols), F32),
            shape((rows, cols), F32),
        ),
        in_specs=[hbm] * 10,
        out_specs=(vmem,) * 6,
        scratch_shapes=[
            VMEM((tokens, width), BF),
            VMEM((tokens, cols), BF),
            VMEM((cols, tokens), BF),
            VMEM((cols, width), BF),
            VMEM((cols, width), BF),
            VMEM((2, n, n, rows // 2, rank), BF),
            VMEM((n, 8, cols), F32),
            VMEM((4, kc), F32),
            VMEM((4, kc), F32),
            VMEM((4, vc), F32),
            VMEM((4, vc), F32),
            VMEM((lines, cols), F32),
            VMEM((lines, cols), F32),
            VMEM((n, lines, cols), BF),
            VMEM((n, lines, cols), BF),
            VMEM((n, lines, cols), BF),
            VMEM((n, 8, 128), F32),
            VMEM((nx * 2, 8, 128), F32),
            DMA((10,)),
        ]
        + [DMA((n,))] * 18
        + [DMA((nx * 2,))] * 2
        + [DMA((n,))] * 2,
        compiler_params=pltpu.CompilerParams(
            collective_id=0, has_side_effects=True, vmem_limit_bytes=40 * 2**20
        ),
    )(*(pltpu.with_memory_space_constraint(array, pltpu.HBM) for array in arrays))
    return pl.pallas_call(
        functools.partial(finish, n),
        name="finish",
        out_shape=(
            shape((rows, kc), F32),
            shape((rows, vc), F32),
            shape((rows, kc), F32),
            shape((rows, vc), F32),
            shape((width, kc), BF),
            shape((width, vc), BF),
            shape((4, kc), F32),
            shape((4, kc), F32),
            shape((4, vc), F32),
            shape((4, vc), F32),
        ),
        in_specs=[vmem] * 6,
        out_specs=(hbm,) * 10,
        scratch_shapes=[
            VMEM((rank, cols), BF),
            VMEM((width, cols), BF),
            VMEM((rows, cols), F32),
            VMEM((rows, cols), F32),
            DMA((2 * (PARTS + 4),)),
        ],
        compiler_params=pltpu.CompilerParams(vmem_limit_bytes=24 * 2**20),
    )(*gathered)


def solution(mesh):
    n = 8
    nx = mesh.devices.size // (2 * n * n)
    torus = Mesh(mesh.devices.reshape(n, n, nx, 2), AXES)
    split = P(FS, TP)
    return jax.shard_map(
        functools.partial(on_device, n, nx),
        mesh=torus,
        in_specs=(P(FS, None), split, split, P(FS, None)) + (split,) * 6,
        out_specs=(split,) * 4 + (P(None, TP),) * 2 + (split,) * 4,
        check_vma=False,
    )
```

```python
import functools

import jax
import jax.numpy as jnp
from jax import lax
from jax.experimental import pallas as pl
from jax.experimental.pallas import tpu as pltpu
from jax.sharding import Mesh
from jax.sharding import PartitionSpec as P

AXES = ("z", "y", "x", "c")
FS = ("z", "y")
TP = ("x", "c")
MESH = pl.DeviceIdType.MESH
VMEM = pltpu.VMEM
DMA = pltpu.SemaphoreType.DMA
BF = jnp.bfloat16
F32 = jnp.float32

learn_rate = 0.05
beta_first = 0.9
beta_second = 0.9
epsilon = 1e-08
norm_eps = 1e-06
PARTS = 4
POINTS = (1, 2, 3, 4)


def permutation(n, c, rank):
    rows = lax.broadcasted_iota(jnp.int32, (rank, rank), 0)
    cols = lax.broadcasted_iota(jnp.int32, (rank, rank), 1)
    r = rows % 4
    low = (rows // 4) % n
    high = rows // (4 * n)
    swapped = (low * n + high) * 4 + r
    wanted = jnp.where(c == 0, swapped, rows)
    return jnp.where(cols == wanted, 1.0, 0.0).astype(BF)


def exchange(
    n,
    nx,
    total,
    normed_h,
    key_h,
    value_h,
    basis_h,
    mk_h,
    mv_h,
    fk_h,
    sk_h,
    fv_h,
    sv_h,
    basis_out,
    m_out,
    d_out,
    nf_out,
    ns_out,
    master_out,
    normed_v,
    cot_v,
    cot_t,
    g_high,
    g_low,
    quarters,
    fk_ref,
    sk_ref,
    fv_ref,
    sv_ref,
    first_own,
    second_own,
    first_all,
    second_all,
    rs_send,
    rs_recv,
    ar_recv,
    ag_recv,
    sq1,
    sq2,
    local_sem,
    b1s,
    b1r,
    b2s,
    b2r,
    xss,
    xsr,
    dds,
    ddr,
    m1s,
    m1r,
    m2s,
    m2r,
    rss,
    rsr,
    ars,
    arr,
    ags,
    agr,
    q1s,
    q1r,
    q2s,
    q2r,
):
    z, y, x, c = (lax.axis_index(name) for name in AXES)
    kc, vc = key_h.shape[1], value_h.shape[1]
    rank = basis_h.shape[1]
    height = basis_h.shape[0]
    half = height // 2
    quarter = height // 4
    lines = 4 * n
    a = y * (1 - c) + z * c
    b = z * (1 - c) + y * c
    t = x * 2 + c
    nt = nx * 2
    h = lax.rem(x, 2)

    def first(d):
        return (lax.rem(z + d * c, n), lax.rem(y + d * (1 - c), n), x, c)

    def second(d):
        return (lax.rem(z + d * (1 - c), n), lax.rem(y + d * c, n), x, c)

    def across(d):
        other = lax.rem(t + d, nt)
        return (z, y, other // 2, lax.rem(other, 2))

    partner = (z, y, x, 1 - c)
    beside = {way: (z, y, lax.rem(x + way + nx, nx), c) for way in (1, -1)}
    started = []

    def send(src, dst, send_sem, recv_sem, device):
        copy = pltpu.make_async_remote_copy(
            src_ref=src,
            dst_ref=dst,
            send_sem=send_sem,
            recv_sem=recv_sem,
            device_id=device,
            device_id_type=MESH,
        )
        copy.start()
        started.append(copy)
        return copy

    def arrived(copies):
        for copy in copies:
            copy.wait_recv()

    mine = quarters.at[c, h, b, a]
    small, large = [
        [pltpu.make_async_copy(src, dst, local_sem.at[k]) for k, src, dst in pairs]
        for pairs in (
            (
                (0, basis_h.at[pl.ds(pl.multiple_of((2 * c + h) * quarter, quarter), quarter)], mine),
                (1, fk_h, fk_ref),
                (2, sk_h, sk_ref),
                (3, fv_h, fv_ref),
                (4, sv_h, sv_ref),
                (5, mk_h, master_out.at[:, pl.ds(0, kc)]),
                (6, mv_h, master_out.at[:, pl.ds(kc, vc)]),
            ),
            (
                (7, key_h, cot_v.at[:, pl.ds(0, kc)]),
                (8, value_h, cot_v.at[:, pl.ds(kc, vc)]),
                (9, normed_h, normed_v),
            ),
        )
    ]
    for copy in small + large:
        copy.start()

    barrier = pltpu.get_barrier_semaphore()
    order = sorted(range(1, n), key=lambda d: -min(d, n - d))
    order_t = range(1, nt)
    for d in range(1, n):
        pl.semaphore_signal(barrier, inc=1, device_id=first(d), device_id_type=MESH)
        pl.semaphore_signal(barrier, inc=1, device_id=second(d), device_id_type=MESH)
    for d in order_t:
        pl.semaphore_signal(barrier, inc=1, device_id=across(d), device_id_type=MESH)

    for copy in small:
        copy.wait()
    first_own[:, :kc] = fk_ref[...]
    first_own[:, kc:] = fv_ref[...]
    second_own[:, :kc] = sk_ref[...]
    second_own[:, kc:] = sv_ref[...]
    m_out[b, a, :height] = master_out[...].astype(BF)
    m_out[b, a, height:] = jnp.concatenate([first_own[...], second_own[...]], axis=0).astype(BF)
    pl.semaphore_wait(barrier, 2 * (n - 1) + nt - 1)

    def onward(away):
        piece = quarters.at[c, h, b, lax.rem(a - away + n, n)]
        for d in order:
            b2[d].append(send(piece, piece, b2s.at[away, d], b2r.at[away, d], second(d)))

    b2 = {d: [] for d in order}
    b1 = {d: send(mine, mine, b1s.at[d], b1r.at[d], first(d)) for d in order}
    onward(0)

    def spread():
        own = m_out.at[b, a]
        return [send(own, own, m1s.at[d], m1r.at[d], first(d)) for d in order]

    m1 = spread()
    for d in reversed(order):
        b1[d].wait_recv()
        onward(d)
    def ring(step, way, part):
        block = lax.rem(b - way * step + n, n)
        where = m_out.at[block] if part is None else m_out.at[block, pl.ds(part * (n // 2), n // 2)]
        k = 2 * step + (0 if way > 0 else 1)
        return send(where, where, m2s.at[k], m2r.at[k], second(way % n))

    rings = []

    def forward(point):
        k = len(rings)
        if k < n // 2 and point in POINTS:
            arrived(rings[-1] if rings else m1)
            last = k == n // 2 - 1
            rings.append([ring(k, 1, 0 if last else None), ring(k, -1, 1 if last else None)])

    dd, xs = [], {}

    def line_of(side, d):
        return quarters.at[c, side, lax.rem(b - d + n, n)]

    def hand_over(d):
        line = line_of(h, d)
        xs[d] = send(line, line, xss.at[d], xsr.at[d], beside[1 if d < n // 2 else -1])
        dd.append(send(line, line, dds.at[0, d], ddr.at[0, d], partner))

    hand_over(0)

    for copy in large:
        copy.wait()
    cot_t[...] = cot_v[...].astype(F32).T.astype(BF)
    wide = normed_v.shape[1]
    step = min(256, wide)

    @pl.loop(0, wide // step)
    def _(i):
        cols = pl.ds(pl.multiple_of(i * step, step), step)
        g = jnp.dot(cot_t[...], normed_v[:, cols], preferred_element_type=F32)
        high = g.astype(BF)
        g_high[:, cols] = high
        g_low[:, cols] = (g - high.astype(F32)).astype(BF)

    for d in reversed(order):
        arrived(b2[d])
        hand_over(d)
    perm = permutation(n, c, rank)
    forward(1)
    for d in [0, *reversed(order)]:
        xs[d].wait_recv()
        line = line_of(1 - h, d)
        dd.append(send(line, line, dds.at[1, d], ddr.at[1, d], partner))
    arrived(dd)
    for zz in range(n):
        for yy in range(n):
            for k in range(2):
                row = (zz * n + yy) * height + k * quarter
                basis_out[row : row + quarter, :] = quarters[0, k, zz, yy]
                basis_out[row + half : row + half + quarter, :] = quarters[1, k, yy, zz]
    low_t = jnp.dot(g_high[...], basis_out[...], preferred_element_type=F32)
    low_t = low_t + jnp.dot(g_low[...], basis_out[...], preferred_element_type=F32)
    flat = lax.dot_general(
        perm, low_t.astype(BF), (((1,), (1,)), ((), ())), preferred_element_type=F32
    ).astype(BF)
    for k in range(n):
        rs_send[k] = flat[k * lines : (k + 1) * lines, :]
    rs_recv[a] = rs_send[a]
    rs = [
        send(rs_send.at[lax.rem(a + d, n)], rs_recv.at[a], rss.at[d], rsr.at[d], first(d))
        for d in order
    ]
    forward(2)
    arrived(rs)
    ar_recv[b] = functools.reduce(jnp.add, [rs_recv[k].astype(F32) for k in range(n)]).astype(BF)
    ar = [send(ar_recv.at[b], ar_recv.at[b], ars.at[d], arr.at[d], second(d)) for d in order]
    forward(3)
    arrived(ar)
    low = functools.reduce(jnp.add, [ar_recv[k].astype(F32) for k in range(n)])
    ag_recv[a] = low.astype(BF)
    squares = low * low
    squares = functools.reduce(
        jnp.add, [squares[8 * k : 8 * k + 8, :] for k in range(lines // 8)]
    )
    squares = functools.reduce(
        jnp.add, [squares[:, 128 * k : 128 * k + 128] for k in range(squares.shape[1] // 128)]
    )
    sq1[a] = squares
    q1 = [send(sq1.at[a], sq1.at[a], q1s.at[d], q1r.at[d], first(d)) for d in order]
    ag = [send(ag_recv.at[a], ag_recv.at[a], ags.at[d], agr.at[d], first(d)) for d in order]
    forward(4)
    arrived(q1)
    sq2[t] = functools.reduce(jnp.add, [sq1[k] for k in range(n)])
    q2 = [send(sq2.at[t], sq2.at[t], q2s.at[d], q2r.at[d], across(d)) for d in order_t]
    while len(rings) < n // 2:
        forward(POINTS[-1])
    arrived(rings[-1])
    for k in range(n):
        for i in range(n):
            row = k * lines + 4 * i
            both = m_out[i, k, height:, :].astype(F32)
            first_all[row : row + 4, :] = both[0:4, :]
            second_all[row : row + 4, :] = both[4:8, :]
    arrived(ag)
    arrived(q2)
    squares = functools.reduce(jnp.add, [sq2[k] for k in range(nt)])
    squares = jnp.sum(jnp.sum(squares, axis=1, keepdims=True), axis=0, keepdims=True)
    grad_scale = 1.0 / jnp.sqrt(squares / total + norm_eps)

    def moved(grad, first_moment, second_moment):
        scaled = grad * grad_scale
        return (
            beta_first * first_moment + (1.0 - beta_first) * scaled,
            beta_second * second_moment + (1.0 - beta_second) * scaled * scaled,
        )

    for k in range(n):
        rows = pl.ds(k * lines, lines)
        new_first, new_second = moved(ag_recv[k].astype(F32), first_all[rows, :], second_all[rows, :])
        d_out[k] = (new_first / (jnp.sqrt(new_second) + epsilon)).astype(BF)
    rows = low[0:4, :]
    for k in range(1, n):
        rows = jnp.where(b == k, low[4 * k : 4 * k + 4, :], rows)
    nf_out[...], ns_out[...] = moved(rows, first_own[...], second_own[...])
    for copy in started:
        copy.wait_send()


def finish(
    n,
    basis_all,
    m_all,
    d_all,
    nf_all,
    ns_all,
    master_own,
    step_key,
    step_value,
    new_key,
    new_value,
    copy_key,
    copy_value,
    nfk,
    nsk,
    nfv,
    nsv,
    directions,
    copies,
    step_v,
    new_v,
    sems,
):
    z, y, c = (lax.axis_index(name) for name in ("z", "y", "c"))
    kc, vc = copy_key.shape[1], copy_value.shape[1]
    rank = basis_all.shape[1]
    height = master_own.shape[0]
    tall = basis_all.shape[0] // PARTS
    started = []

    def put(src, key_dst, value_dst):
        for dst, cols in ((key_dst, pl.ds(0, kc)), (value_dst, pl.ds(kc, vc))):
            copy = pltpu.make_async_copy(src.at[:, cols], dst, sems.at[len(started)])
            copy.start()
            started.append(copy)

    put(nf_all, nfk, nfv)
    put(ns_all, nsk, nsv)
    flat = d_all[...].reshape(rank, d_all.shape[2])
    directions[...] = jnp.dot(permutation(n, c, rank), flat, preferred_element_type=F32).astype(BF)
    for i in range(PARTS):
        rows = pl.ds(i * tall, tall)
        part = jnp.dot(basis_all[rows, :], directions[...], preferred_element_type=F32)
        for k in range(tall // height):
            block = i * (tall // height) + k
            high, low = block // n, block % n
            master = m_all[high * (1 - c) + low * c, low * (1 - c) + high * c, :height].astype(F32)
            moved = master - learn_rate * part[k * height : (k + 1) * height, :]
            copies[block * height : (block + 1) * height, :] = moved.astype(BF)
        put(copies.at[rows], copy_key.at[rows], copy_value.at[rows])
    mine = pl.ds(pl.multiple_of((z * n + y) * height, height), height)
    own = jnp.dot(basis_all[mine, :], directions[...], preferred_element_type=F32)
    step_v[...] = own
    new_v[...] = master_own[...] - learn_rate * own
    put(step_v, step_key, step_value)
    put(new_v, new_key, new_value)
    for copy in started:
        copy.wait()


def on_device(n, nx, *arrays):
    normed, key_cot, value_cot, basis = arrays[:4]
    kc, vc = key_cot.shape[1], value_cot.shape[1]
    cols = kc + vc
    rows, rank = basis.shape
    tokens, width = normed.shape
    total = rank * cols * nx * 2
    hbm = pl.BlockSpec(memory_space=pltpu.HBM)
    vmem = pl.BlockSpec(memory_space=VMEM)
    shape = jax.ShapeDtypeStruct
    lines = 4 * n
    gathered = pl.pallas_call(
        functools.partial(exchange, n, nx, total),
        name="exchange",
        out_shape=(
            shape((width, rank), BF),
            shape((n, n, rows + 8, cols), BF),
            shape((n, lines, cols), BF),
            shape((4, cols), F32),
            shape((4, cols), F32),
            shape((rows, cols), F32),
        ),
        in_specs=[hbm] * 10,
        out_specs=(vmem,) * 6,
        scratch_shapes=[
            VMEM((tokens, width), BF),
            VMEM((tokens, cols), BF),
            VMEM((cols, tokens), BF),
            VMEM((cols, width), BF),
            VMEM((cols, width), BF),
            VMEM((2, 2, n, n, rows // 4, rank), BF),
            VMEM((4, kc), F32),
            VMEM((4, kc), F32),
            VMEM((4, vc), F32),
            VMEM((4, vc), F32),
            VMEM((4, cols), F32),
            VMEM((4, cols), F32),
            VMEM((rank, cols), F32),
            VMEM((rank, cols), F32),
            VMEM((n, lines, cols), BF),
            VMEM((n, lines, cols), BF),
            VMEM((n, lines, cols), BF),
            VMEM((n, lines, cols), BF),
            VMEM((n, 8, 128), F32),
            VMEM((nx * 2, 8, 128), F32),
            DMA((10,)),
        ]
        + [DMA((n,))] * 2
        + [DMA((n, n))] * 2
        + [DMA((n,))] * 2
        + [DMA((2, n))] * 2
        + [DMA((n,))] * 12
        + [DMA((nx * 2,))] * 2,
        compiler_params=pltpu.CompilerParams(
            collective_id=0, has_side_effects=True, vmem_limit_bytes=40 * 2**20
        ),
    )(*(pltpu.with_memory_space_constraint(array, pltpu.HBM) for array in arrays))
    return pl.pallas_call(
        functools.partial(finish, n),
        name="finish",
        out_shape=(
            shape((rows, kc), F32),
            shape((rows, vc), F32),
            shape((rows, kc), F32),
            shape((rows, vc), F32),
            shape((width, kc), BF),
            shape((width, vc), BF),
            shape((4, kc), F32),
            shape((4, kc), F32),
            shape((4, vc), F32),
            shape((4, vc), F32),
        ),
        in_specs=[vmem] * 6,
        out_specs=(hbm,) * 10,
        scratch_shapes=[
            VMEM((rank, cols), BF),
            VMEM((width, cols), BF),
            VMEM((rows, cols), F32),
            VMEM((rows, cols), F32),
            DMA((2 * (PARTS + 4),)),
        ],
        compiler_params=pltpu.CompilerParams(vmem_limit_bytes=24 * 2**20),
    )(*gathered)


def solution(mesh):
    n = 8
    nx = mesh.devices.size // (2 * n * n)
    torus = Mesh(mesh.devices.reshape(n, n, nx, 2), AXES)
    split = P(FS, TP)
    return jax.shard_map(
        functools.partial(on_device, n, nx),
        mesh=torus,
        in_specs=(P(FS, None), split, split, P(FS, None)) + (split,) * 6,
        out_specs=(split,) * 4 + (P(None, TP),) * 2 + (split,) * 4,
        check_vma=False,
    )
```

```python
import functools

import jax
import jax.numpy as jnp
from jax import lax
from jax.experimental import pallas as pl
from jax.experimental.pallas import tpu as pltpu
from jax.sharding import Mesh
from jax.sharding import PartitionSpec as P

AXES = ("z", "y", "x", "c")
FS = ("z", "y")
TP = ("x", "c")
MESH = pl.DeviceIdType.MESH
VMEM = pltpu.VMEM
DMA = pltpu.SemaphoreType.DMA
BF = jnp.bfloat16
F32 = jnp.float32

learn_rate = 0.05
beta_first = 0.9
beta_second = 0.9
epsilon = 1e-08
norm_eps = 1e-06
PARTS = 4
POINTS = (1, 2, 3)


def permutation(n, c, rank):
    rows = lax.broadcasted_iota(jnp.int32, (rank, rank), 0)
    cols = lax.broadcasted_iota(jnp.int32, (rank, rank), 1)
    r = rows % 4
    low = (rows // 4) % n
    high = rows // (4 * n)
    swapped = (low * n + high) * 4 + r
    wanted = jnp.where(c == 0, swapped, rows)
    return jnp.where(cols == wanted, 1.0, 0.0).astype(BF)


def exchange(
    n,
    nx,
    total,
    normed_h,
    key_h,
    value_h,
    basis_h,
    mk_h,
    mv_h,
    fk_h,
    sk_h,
    fv_h,
    sv_h,
    basis_out,
    m_out,
    d_out,
    nf_out,
    ns_out,
    master_out,
    normed_v,
    cot_v,
    cot_t,
    g_high,
    g_low,
    quarters,
    fk_ref,
    sk_ref,
    fv_ref,
    sv_ref,
    first_own,
    second_own,
    first_all,
    second_all,
    rs_send,
    rs_recv,
    ar_recv,
    ag_recv,
    sq1,
    sq2,
    local_sem,
    b1s,
    b1r,
    b2s,
    b2r,
    xss,
    xsr,
    dds,
    ddr,
    m1s,
    m1r,
    m2s,
    m2r,
    rss,
    rsr,
    ars,
    arr,
    ags,
    agr,
    q1s,
    q1r,
    q2s,
    q2r,
):
    z, y, x, c = (lax.axis_index(name) for name in AXES)
    kc, vc = key_h.shape[1], value_h.shape[1]
    rank = basis_h.shape[1]
    height = basis_h.shape[0]
    half = height // 2
    quarter = height // 4
    lines = 4 * n
    a = y * (1 - c) + z * c
    b = z * (1 - c) + y * c
    h = lax.rem(x, 2)

    def first(d):
        return (lax.rem(z + d * c, n), lax.rem(y + d * (1 - c), n), x, c)

    def second(d):
        return (lax.rem(z + d * (1 - c), n), lax.rem(y + d * c, n), x, c)

    def plane(dx, d):
        return (lax.rem(z + d * c, n), lax.rem(y + d * (1 - c), n), lax.rem(x + dx, nx), c)

    partner = (z, y, x, 1 - c)
    beside = {way: (z, y, lax.rem(x + way + nx, nx), c) for way in (1, -1)}
    started = []

    def send(src, dst, send_sem, recv_sem, device):
        copy = pltpu.make_async_remote_copy(
            src_ref=src,
            dst_ref=dst,
            send_sem=send_sem,
            recv_sem=recv_sem,
            device_id=device,
            device_id_type=MESH,
        )
        copy.start()
        started.append(copy)
        return copy

    def arrived(copies):
        for copy in copies:
            copy.wait_recv()

    mine = quarters.at[c, h, b, a]
    small, large = [
        [pltpu.make_async_copy(src, dst, local_sem.at[k]) for k, src, dst in pairs]
        for pairs in (
            (
                (0, basis_h.at[pl.ds(pl.multiple_of((2 * c + h) * quarter, quarter), quarter)], mine),
                (1, fk_h, fk_ref),
                (2, sk_h, sk_ref),
                (3, fv_h, fv_ref),
                (4, sv_h, sv_ref),
                (5, mk_h, master_out.at[:, pl.ds(0, kc)]),
                (6, mv_h, master_out.at[:, pl.ds(kc, vc)]),
            ),
            (
                (7, key_h, cot_v.at[:, pl.ds(0, kc)]),
                (8, value_h, cot_v.at[:, pl.ds(kc, vc)]),
                (9, normed_h, normed_v),
            ),
        )
    ]
    for copy in small + large:
        copy.start()

    barrier = pltpu.get_barrier_semaphore()
    order = sorted(range(1, n), key=lambda d: -min(d, n - d))
    plane_order = [(dx, d) for dx in range(nx) for d in [*order, 0] if dx or d]
    for peer in (
        [plane(dx, d) for dx, d in plane_order] + [second(d) for d in order] + [partner]
    ):
        pl.semaphore_signal(barrier, inc=1, device_id=peer, device_id_type=MESH)

    for copy in small:
        copy.wait()
    first_own[:, :kc] = fk_ref[...]
    first_own[:, kc:] = fv_ref[...]
    second_own[:, :kc] = sk_ref[...]
    second_own[:, kc:] = sv_ref[...]
    m_out[b, a, :height] = master_out[...].astype(BF)
    m_out[b, a, height:] = jnp.concatenate([first_own[...], second_own[...]], axis=0).astype(BF)
    pl.semaphore_wait(barrier, len(plane_order) + n)

    def onward(away):
        piece = quarters.at[c, h, b, lax.rem(a - away + n, n)]
        for d in order:
            b2[d].append(send(piece, piece, b2s.at[away, d], b2r.at[away, d], second(d)))

    b2 = {d: [] for d in order}
    b1 = {d: send(mine, mine, b1s.at[d], b1r.at[d], first(d)) for d in order}
    onward(0)

    def spread():
        own = m_out.at[b, a]
        return [send(own, own, m1s.at[d], m1r.at[d], first(d)) for d in order]

    m1 = spread()

    for copy in large:
        copy.wait()
    cot_t[...] = cot_v[...].astype(F32).T.astype(BF)
    wide = normed_v.shape[1]
    step = min(256, wide)

    def local_gradient(i):
        cols = pl.ds(pl.multiple_of(i * step, step), step)
        g = jnp.dot(cot_t[...], normed_v[:, cols], preferred_element_type=F32)
        high = g.astype(BF)
        g_high[:, cols] = high
        g_low[:, cols] = (g - high.astype(F32)).astype(BF)

    pl.loop(0, wide // step // 2)(local_gradient)

    for d in reversed(order):
        b1[d].wait_recv()
        onward(d)
    def ring(step, way, hops, part):
        block = lax.rem(b - way * step + n, n)
        where = m_out.at[block] if part is None else m_out.at[block, pl.ds(part * (n // 2), n // 2)]
        k = 4 * step + (0 if way > 0 else 1) + (0 if part is None else 2)
        return send(where, where, m2s.at[k], m2r.at[k], second(way * hops % n))

    rings, last = [], max(n // 2 - 2, 0)

    def forward(point):
        k = len(rings)
        if k <= last and point in POINTS:
            arrived(rings[-1] if rings else m1)
            rings.append([])
            if n > 2:
                rings[-1] += [ring(k, 1, 1, None), ring(k, -1, 1, None)]
            if k == last:
                far = min(2, n // 2)
                rings[-1] += [ring(n // 2 - far, 1, far, 0), ring(n // 2 - far, -1, far, 1)]

    dd, xs = [], {}

    def line_of(side, d):
        return quarters.at[c, side, lax.rem(b - d + n, n)]

    def hand_over(d):
        line = line_of(h, d)
        xs[d] = send(line, line, xss.at[d], xsr.at[d], beside[1 if d < n // 2 else -1])
        dd.append(send(line, line, dds.at[0, d], ddr.at[0, d], partner))

    hand_over(0)

    pl.loop(wide // step // 2, wide // step)(local_gradient)
    for d in reversed(order):
        arrived(b2[d])
        hand_over(d)
    perm = permutation(n, c, rank)
    forward(1)
    for d in [0, *reversed(order)]:
        xs[d].wait_recv()
        line = line_of(1 - h, d)
        dd.append(send(line, line, dds.at[1, d], ddr.at[1, d], partner))
    arrived(dd)
    for zz in range(n):
        for yy in range(n):
            for k in range(2):
                row = (zz * n + yy) * height + k * quarter
                basis_out[row : row + quarter, :] = quarters[0, k, zz, yy]
                basis_out[row + half : row + half + quarter, :] = quarters[1, k, yy, zz]
    low_t = jnp.dot(g_high[...], basis_out[...], preferred_element_type=F32)
    low_t = low_t + jnp.dot(g_low[...], basis_out[...], preferred_element_type=F32)
    flat = lax.dot_general(
        perm, low_t.astype(BF), (((1,), (1,)), ((), ())), preferred_element_type=F32
    ).astype(BF)
    for k in range(n):
        rs_send[k] = flat[k * lines : (k + 1) * lines, :]
    rs_recv[a] = rs_send[a]
    rs = [
        send(rs_send.at[lax.rem(a + d, n)], rs_recv.at[a], rss.at[d], rsr.at[d], first(d))
        for d in order
    ]
    forward(2)
    arrived(rs)
    ar_recv[b] = functools.reduce(jnp.add, [rs_recv[k].astype(F32) for k in range(n)]).astype(BF)
    ar = [send(ar_recv.at[b], ar_recv.at[b], ars.at[d], arr.at[d], second(d)) for d in order]
    forward(3)
    arrived(ar)
    low = functools.reduce(jnp.add, [ar_recv[k].astype(F32) for k in range(n)])
    ag_recv[a] = low.astype(BF)
    squares = low * low
    squares = functools.reduce(
        jnp.add, [squares[8 * k : 8 * k + 8, :] for k in range(lines // 8)]
    )
    squares = functools.reduce(
        jnp.add, [squares[:, 128 * k : 128 * k + 128] for k in range(squares.shape[1] // 128)]
    )
    sq1[x, a] = jnp.sum(squares, axis=0, keepdims=True)
    q1 = [
        send(sq1.at[x, a], sq1.at[x, a], q1s.at[dx, d], q1r.at[dx, d], plane(dx, d))
        for dx, d in plane_order
    ]
    ag = [send(ag_recv.at[a], ag_recv.at[a], ags.at[d], agr.at[d], first(d)) for d in order]
    forward(4)
    arrived(q1)
    sq2[c] = functools.reduce(jnp.add, [sq1[k, i] for k in range(nx) for i in range(n)])
    q2 = [send(sq2.at[c], sq2.at[c], q2s.at[0], q2r.at[0], partner)]
    while len(rings) <= last:
        forward(POINTS[-1])
    arrived(rings[-1])
    for k in range(n):
        for i in range(n):
            row = k * lines + 4 * i
            both = m_out[i, k, height:, :].astype(F32)
            first_all[row : row + 4, :] = both[0:4, :]
            second_all[row : row + 4, :] = both[4:8, :]
    arrived(ag)
    arrived(q2)
    squares = jnp.sum(sq2[0] + sq2[1], axis=1, keepdims=True)
    grad_scale = 1.0 / jnp.sqrt(squares / total + norm_eps)

    def moved(grad, first_moment, second_moment):
        scaled = grad * grad_scale
        return (
            beta_first * first_moment + (1.0 - beta_first) * scaled,
            beta_second * second_moment + (1.0 - beta_second) * scaled * scaled,
        )

    for k in range(n):
        rows = pl.ds(k * lines, lines)
        new_first, new_second = moved(ag_recv[k].astype(F32), first_all[rows, :], second_all[rows, :])
        d_out[k] = (new_first / (jnp.sqrt(new_second) + epsilon)).astype(BF)
    rows = low[0:4, :]
    for k in range(1, n):
        rows = jnp.where(b == k, low[4 * k : 4 * k + 4, :], rows)
    nf_out[...], ns_out[...] = moved(rows, first_own[...], second_own[...])
    for copy in started:
        copy.wait_send()


def finish(
    n,
    basis_all,
    m_all,
    d_all,
    nf_all,
    ns_all,
    master_own,
    step_key,
    step_value,
    new_key,
    new_value,
    copy_key,
    copy_value,
    nfk,
    nsk,
    nfv,
    nsv,
    directions,
    copies,
    step_v,
    new_v,
    sems,
):
    z, y, c = (lax.axis_index(name) for name in ("z", "y", "c"))
    kc, vc = copy_key.shape[1], copy_value.shape[1]
    rank = basis_all.shape[1]
    height = master_own.shape[0]
    tall = basis_all.shape[0] // PARTS
    started = []

    def put(src, key_dst, value_dst):
        for dst, cols in ((key_dst, pl.ds(0, kc)), (value_dst, pl.ds(kc, vc))):
            copy = pltpu.make_async_copy(src.at[:, cols], dst, sems.at[len(started)])
            copy.start()
            started.append(copy)

    put(nf_all, nfk, nfv)
    put(ns_all, nsk, nsv)
    flat = d_all[...].reshape(rank, d_all.shape[2])
    directions[...] = jnp.dot(permutation(n, c, rank), flat, preferred_element_type=F32).astype(BF)
    for i in range(PARTS):
        rows = pl.ds(i * tall, tall)
        part = jnp.dot(basis_all[rows, :], directions[...], preferred_element_type=F32)
        for k in range(tall // height):
            block = i * (tall // height) + k
            high, low = block // n, block % n
            master = m_all[high * (1 - c) + low * c, low * (1 - c) + high * c, :height].astype(F32)
            moved = master - learn_rate * part[k * height : (k + 1) * height, :]
            copies[block * height : (block + 1) * height, :] = moved.astype(BF)
        put(copies.at[rows], copy_key.at[rows], copy_value.at[rows])
    mine = pl.ds(pl.multiple_of((z * n + y) * height, height), height)
    own = jnp.dot(basis_all[mine, :], directions[...], preferred_element_type=F32)
    step_v[...] = own
    new_v[...] = master_own[...] - learn_rate * own
    put(step_v, step_key, step_value)
    put(new_v, new_key, new_value)
    for copy in started:
        copy.wait()


def on_device(n, nx, *arrays):
    normed, key_cot, value_cot, basis = arrays[:4]
    kc, vc = key_cot.shape[1], value_cot.shape[1]
    cols = kc + vc
    rows, rank = basis.shape
    tokens, width = normed.shape
    total = rank * cols * nx * 2
    hbm = pl.BlockSpec(memory_space=pltpu.HBM)
    vmem = pl.BlockSpec(memory_space=VMEM)
    shape = jax.ShapeDtypeStruct
    lines = 4 * n
    gathered = pl.pallas_call(
        functools.partial(exchange, n, nx, total),
        name="exchange",
        out_shape=(
            shape((width, rank), BF),
            shape((n, n, rows + 8, cols), BF),
            shape((n, lines, cols), BF),
            shape((4, cols), F32),
            shape((4, cols), F32),
            shape((rows, cols), F32),
        ),
        in_specs=[hbm] * 10,
        out_specs=(vmem,) * 6,
        scratch_shapes=[
            VMEM((tokens, width), BF),
            VMEM((tokens, cols), BF),
            VMEM((cols, tokens), BF),
            VMEM((cols, width), BF),
            VMEM((cols, width), BF),
            VMEM((2, 2, n, n, rows // 4, rank), BF),
            VMEM((4, kc), F32),
            VMEM((4, kc), F32),
            VMEM((4, vc), F32),
            VMEM((4, vc), F32),
            VMEM((4, cols), F32),
            VMEM((4, cols), F32),
            VMEM((rank, cols), F32),
            VMEM((rank, cols), F32),
            VMEM((n, lines, cols), BF),
            VMEM((n, lines, cols), BF),
            VMEM((n, lines, cols), BF),
            VMEM((n, lines, cols), BF),
            VMEM((nx, n, 1, 128), F32),
            VMEM((2, 1, 128), F32),
            DMA((10,)),
        ]
        + [DMA((n,))] * 2
        + [DMA((n, n))] * 2
        + [DMA((n,))] * 2
        + [DMA((2, n))] * 2
        + [DMA((n,))] * 2
        + [DMA((2 * n,))] * 2
        + [DMA((n,))] * 6
        + [DMA((nx, n))] * 2
        + [DMA((1,))] * 2,
        compiler_params=pltpu.CompilerParams(
            collective_id=0, has_side_effects=True, vmem_limit_bytes=40 * 2**20
        ),
    )(*(pltpu.with_memory_space_constraint(array, pltpu.HBM) for array in arrays))
    return pl.pallas_call(
        functools.partial(finish, n),
        name="finish",
        out_shape=(
            shape((rows, kc), F32),
            shape((rows, vc), F32),
            shape((rows, kc), F32),
            shape((rows, vc), F32),
            shape((width, kc), BF),
            shape((width, vc), BF),
            shape((4, kc), F32),
            shape((4, kc), F32),
            shape((4, vc), F32),
            shape((4, vc), F32),
        ),
        in_specs=[vmem] * 6,
        out_specs=(hbm,) * 10,
        scratch_shapes=[
            VMEM((rank, cols), BF),
            VMEM((width, cols), BF),
            VMEM((rows, cols), F32),
            VMEM((rows, cols), F32),
            DMA((2 * (PARTS + 4),)),
        ],
        compiler_params=pltpu.CompilerParams(vmem_limit_bytes=24 * 2**20),
    )(*gathered)


def solution(mesh):
    n = 8
    nx = mesh.devices.size // (2 * n * n)
    torus = Mesh(mesh.devices.reshape(n, n, nx, 2), AXES)
    split = P(FS, TP)
    return jax.shard_map(
        functools.partial(on_device, n, nx),
        mesh=torus,
        in_specs=(P(FS, None), split, split, P(FS, None)) + (split,) * 6,
        out_specs=(split,) * 4 + (P(None, TP),) * 2 + (split,) * 4,
        check_vma=False,
    )
```
